32 devices in a mesh: grp: 2 (over x), ep: 8 (over z, y), tp: 2 (over core).
Axes of the slice: x: 2, y: 2, z: 4, core: 2. Of those that a mesh axis runs over, the one named last changes fastest.
Arguments:
- tokens: bfloat16 [4096, 2048], P(('grp', 'ep')), parts along dimension 0, may hold values from -6 to 6
- picks: int32 [8, 512], P(None, ('grp', 'ep')), parts along dimension 1, may hold values from 0 to 2047, as said below
- route_weights: bfloat16 [8, 512], P(None, ('grp', 'ep')), parts along dimension 1, may hold values from 0.19921875 to 1
- gate_weight: bfloat16 [8, 2048, 1024], P('ep', None, 'tp'), may hold values from -0.125 to 0.125
- up_weight: bfloat16 [8, 2048, 1024], P('ep', None, 'tp'), may hold values from -0.125 to 0.125
- down_weight: bfloat16 [8, 1024, 2048], P('ep', 'tp'), may hold values from -0.1875 to 0.1875
Outputs:
- mixed: bfloat16 [4096, 2048], P(('grp', 'ep'), 'tp'), parts along dimension 0
The draws below stay inside these ranges and needn't reach their ends.
There are 2 independent parts, one for each index of `grp`. The reference program is written for one: setup_inputs(seed, part) draws one part's arguments, and reference() takes and returns one part's arrays. A program takes and returns all parts, laid end to end along the dimension named above; an argument that names none is the same for every part. Nothing has to cross between parts.
Inputs may be any that keep to these rules, and one draw needn't show every extreme that they name: `picks`: slots k * 32 to (k + 1) * 32 - 1 of every expert name 32 different tokens of the block k * 256 to (k + 1) * 256 - 1.
All inputs are finite; a program needn't handle non-finite values.
Results may differ from the reference program's by a relative error of at most 0.0066.
Values may be sent and summed in bfloat16 or wider, within the bound.
No kernel may reach another device: no remote copies, remote signals or barrier semaphores. Data moves between devices by JAX's collectives and lax.ppermute only.
A program may use at most 64 MiB of HBM per device.

```python
import jax
import jax.numpy as jnp
from jax import lax

D = 2048
FF = 1024
TOK_DEV = 256
PER = 32
EXPERTS = 8
CAP = 256
TOKENS = 2048
N_TP = 2


def draw_picks(key, part):
    sources = TOKENS // TOK_DEV
    keys = jax.random.split(jax.random.fold_in(key, 7), EXPERTS * sources)
    chosen = jax.vmap(lambda single: jax.random.permutation(single, TOK_DEV)[:PER])(keys)
    offsets = jnp.arange(sources, dtype=jnp.int32) * TOK_DEV
    chosen = chosen.astype(jnp.int32).reshape(EXPERTS, sources, PER) + offsets[None, :, None]
    return chosen.reshape(EXPERTS, sources * PER).astype(jnp.int32)


def block_levels(rng, extent, pieces, low, largest):
    level, own = 1.0, jax.random.fold_in(rng, 6)
    for axis_at, blocks in pieces:
        steps = jnp.exp(jax.random.uniform(jax.random.fold_in(own, axis_at), (blocks,), jnp.float32, low / len(pieces), largest / len(pieces)))
        level = level * jnp.repeat(steps, extent[axis_at] // blocks).reshape([-1 if axis == axis_at else 1 for axis in range(len(extent))])
    return level


def noise(rng, shape, scale, most, pieces=(), kind=jnp.bfloat16):
    loudness = block_levels(rng, shape, pieces, -0.22, 0.18) if pieces else 1.0
    array = jax.random.normal(rng, shape, jnp.float32) * scale * loudness
    return jnp.minimum(jnp.maximum(array, -most), most).astype(kind)


def setup_inputs(seed: int = 0, part: int = 0) -> dict:
    streams_of = jax.random.split(jax.random.key(seed), 7)
    part_splits = jax.random.split(jax.random.fold_in(streams_of[6], part), 7)
    tokens = noise(part_splits[0], (TOKENS, D), 1.0, 6.0, ((0, 8),))
    picks = draw_picks(jax.random.fold_in(jax.random.fold_in(streams_of[6], part), 71), part)
    route_weights = jnp.clip(0.19921875 + 0.80078125 * jax.random.uniform(part_splits[2], (EXPERTS, CAP), jnp.float32) ** block_levels(part_splits[2], (EXPERTS, CAP), ((1, 8),), -0.2, 0.2), 0.19921875, 1.0).astype(jnp.bfloat16)
    gate_weight = noise(streams_of[3], (EXPERTS, D, FF), D ** -0.5, 0.125, ((0, 8), (2, 2)))
    up_weight = noise(streams_of[4], (EXPERTS, D, FF), D ** -0.5, 0.125, ((0, 8), (2, 2)))
    down_weight = noise(streams_of[5], (EXPERTS, FF, D), FF ** -0.5, 0.1875, ((0, 8), (1, 2)))
    return dict(tokens=tokens, picks=picks, route_weights=route_weights, gate_weight=gate_weight, up_weight=up_weight, down_weight=down_weight)


def reference(tokens, picks, route_weights, gate_weight, up_weight, down_weight):
    half_width = FF // N_TP

    def one_expert(total, index):
        rows = jnp.take(tokens, picks[index], axis=0)
        gate = jnp.dot(rows, gate_weight[index], preferred_element_type=jnp.float32)
        up = jnp.dot(rows, up_weight[index], preferred_element_type=jnp.float32)
        scale = route_weights[index].astype(jnp.float32)[:, None]
        hidden = (jax.nn.silu(gate) * up * scale).astype(jnp.bfloat16)
        summed = jnp.zeros((rows.shape[0], D), jnp.float32)
        for block in range(N_TP):
            left = hidden[:, block * half_width:(block + 1) * half_width]
            right = down_weight[index, block * half_width:(block + 1) * half_width]
            partial_value = jnp.dot(left, right, preferred_element_type=jnp.float32).astype(jnp.bfloat16)
            summed = summed + partial_value.astype(jnp.float32)
        result = summed.astype(jnp.bfloat16).astype(jnp.float32)
        return total.at[picks[index]].add(result), None

    start = jnp.zeros((TOKENS, D), jnp.float32)
    total, _ = lax.scan(one_expert, start, jnp.arange(EXPERTS, dtype=jnp.int32))
    return total.astype(jnp.bfloat16)
```

```python
import functools

import jax
import jax.numpy as jnp
from jax import lax
from jax.experimental import pallas as pl
from jax.experimental.pallas import tpu as pltpu
from jax.sharding import PartitionSpec as P

VMEM = pl.BlockSpec(memory_space=pltpu.VMEM)
HBM = pl.BlockSpec(memory_space=pltpu.HBM)
F32 = jnp.float32
BF16 = jnp.bfloat16


def far_first(count):
    order, top = [], count // 2
    while top >= 1:
        order += range(top, 2 * top)
        top //= 2
    return order


def select_rows(ids, tokens):
    at = lax.broadcasted_iota(jnp.int32, (tokens.shape[0], ids.shape[1]), 0)
    onehot = (at == ids).astype(F32).astype(BF16)
    return lax.dot_general(
        onehot, tokens, (((0,), (0,)), ((), ())), preferred_element_type=F32
    ).astype(BF16)


def gather_kernel(far, picks_ref, tokens_ref, *outs):
    block = tokens_ref.shape[0]
    me, core = lax.axis_index("ep"), lax.axis_index("tp")
    tokens = tokens_ref[...]
    half = picks_ref.shape[1] // 2

    def ids_of(expert):
        return lax.rem(picks_ref[pl.ds(expert, 1), :], block)

    for pair, out in zip(far, outs):
        out[...] = select_rows(ids_of(me ^ (2 * pair + core)), tokens)
    near = select_rows(ids_of(me ^ 1), tokens)
    near_out, own_out = outs[-2:]
    near_out[...] = jnp.where(core == 0, near[:half], near[half:])
    own_out[...] = select_rows(ids_of(me), tokens)


def fetch_kernel(*refs):
    half = len(refs) // 2
    sems = refs[-1]
    pairs = list(zip(refs[:half], refs[half:-1]))
    for i, (src, dst) in enumerate(pairs):
        pltpu.make_async_copy(src, dst, sems.at[i]).start()
    for i, (src, dst) in enumerate(pairs):
        pltpu.make_async_copy(src, dst, sems.at[i]).wait()


def expert_kernel(count, *refs):
    gate_ref, up_ref, down_ref = refs[:3]
    own_ref, near_mine, near_other = refs[3:6]
    blocks = refs[6:6 + count - 2]
    keep_ref, send_ref, rows = refs[6 + count - 2:]
    core = lax.axis_index("tp")
    per = own_ref.shape[0]
    half = per // 2
    rows[:per, :] = own_ref[...]
    mine, other = near_mine[...], near_other[...]
    rows[per:per + half, :] = jnp.where(core == 0, mine, other)
    rows[per + half:2 * per, :] = jnp.where(core == 0, other, mine)
    pairs = count // 2 - 1
    for a in range(pairs):
        ours, theirs = blocks[a][...], blocks[pairs + a][...]
        rows[(2 + 2 * a) * per:(3 + 2 * a) * per, :] = jnp.where(core == 0, ours, theirs)
        rows[(3 + 2 * a) * per:(4 + 2 * a) * per, :] = jnp.where(core == 0, theirs, ours)
    x = rows[...]
    gate = jnp.dot(x, gate_ref[...], preferred_element_type=F32)
    up = jnp.dot(x, up_ref[...], preferred_element_type=F32)
    hidden = (gate / (1.0 + jnp.exp(-gate)) * up).astype(BF16)
    width = keep_ref.shape[1]
    for offset, out in ((1 - core, send_ref), (core, keep_ref)):
        columns = pl.ds(pl.multiple_of(offset * width, width), width)
        out[...] = jnp.dot(hidden, down_ref[:, columns], preferred_element_type=F32).astype(BF16)


def add_kernel(keep_ref, got_ref, *outs):
    per = outs[0].shape[0]
    for m, out in enumerate(outs):
        span = slice(m * per, (m + 1) * per)
        out[...] = (keep_ref[span, :].astype(F32) + got_ref[span, :].astype(F32)).astype(BF16)


def combine_kernel(picks_ref, weights_ref, *refs):
    blocks, out_ref, flat, mix = refs[:-3], refs[-3], refs[-2], refs[-1]
    me = lax.axis_index("ep")
    tokens, per = out_ref.shape[0], blocks[0].shape[0]
    for m, block in enumerate(blocks):
        expert = me ^ m
        flat[pl.ds(pl.multiple_of(expert * per, per), per), :] = block[...]
    at = lax.broadcasted_iota(jnp.int32, (tokens, picks_ref.shape[1]), 0)
    ids = lax.rem(picks_ref[...], tokens)
    mix[...] = jnp.where(at == ids, weights_ref[...].astype(F32), 0.0).astype(BF16)
    out_ref[...] = jnp.dot(mix[...], flat[...], preferred_element_type=F32).astype(BF16)


def call(kernel, name, outs, specs, scratch=(), flops=0, nbytes=0):
    return pl.pallas_call(
        kernel,
        name=name,
        out_shape=outs,
        in_specs=specs,
        out_specs=jax.tree.map(lambda _: VMEM, outs),
        scratch_shapes=list(scratch),
        cost_estimate=pl.CostEstimate(flops=flops, transcendentals=0, bytes_accessed=nbytes),
        compiler_params=pltpu.CompilerParams(vmem_limit_bytes=40 << 20),
    )


def shape(*dims, dtype=BF16):
    return jax.ShapeDtypeStruct(dims, dtype)


def per_device(tokens, picks, route_weights, gate_weight, up_weight, down_weight):
    count, cores = lax.axis_size("ep"), lax.axis_size("tp")
    experts, per = picks.shape
    block, width = tokens.shape
    if experts != count or cores != 2 or count & (count - 1) or count < 4:
        raise ValueError("unsupported mesh")
    wide = width // cores
    gate_weight, up_weight, down_weight = gate_weight[0], up_weight[0], down_weight[0]
    pairs = far_first(count // 2)

    def exchange(value, mask):
        return lax.ppermute(value, "ep", [(i, i ^ mask) for i in range(count)])

    def exchange_pair(value, pair):
        hops = [(i * 2 + t, (i ^ (2 * pair + t)) * 2 + t) for i in range(count) for t in range(2)]
        return lax.ppermute(value, ("ep", "tp"), hops)

    def swap(value):
        return lax.ppermute(value, "tp", [(0, 1), (1, 0)])

    n_far = len(pairs)
    sent = call(
        functools.partial(gather_kernel, pairs),
        "gather",
        [shape(per, width)] * n_far + [shape(per // 2, width), shape(per, width)],
        [VMEM, VMEM],
    )(picks, tokens)
    got = {pair: exchange_pair(value, pair) for pair, value in zip(pairs, sent)}
    near, own = exchange(sent[-2], 1), sent[-1]
    other = {pair: swap(got[pair]) for pair in pairs}
    near_other = swap(near)

    weights = call(
        fetch_kernel,
        "fetch",
        [pltpu.VMEM(w.shape, w.dtype) for w in (gate_weight, up_weight, down_weight)],
        [HBM] * 3,
        [pltpu.SemaphoreType.DMA((3,))],
        nbytes=6 << 20,
    )(gate_weight, up_weight, down_weight)

    order = sorted(pairs)
    keep, send = call(
        functools.partial(expert_kernel, count),
        "expert",
        [shape(count * per, wide)] * 2,
        [VMEM] * (6 + 2 * n_far),
        [pltpu.VMEM((count * per, width), BF16)],
        flops=2 * 3 * count * per * width * gate_weight.shape[1],
    )(*weights, own, near, near_other, *[got[a] for a in order], *[other[a] for a in order])
    received = swap(send)
    results = call(
        add_kernel, "add", [shape(per, wide)] * count, [VMEM, VMEM],
    )(keep, received)
    returned = [results[0]] + [None] * (count - 1)
    for mask in far_first(count):
        returned[mask] = exchange(results[mask], mask)
    return call(
        combine_kernel,
        "combine",
        shape(block, wide),
        [VMEM] * (2 + count),
        [pltpu.VMEM((count * per, wide), BF16), pltpu.VMEM((block, count * per), BF16)],
    )(picks.reshape(1, experts * per), route_weights.reshape(1, experts * per), *returned)


def solution(mesh):
    return jax.shard_map(
        per_device,
        mesh=mesh,
        in_specs=(
            P(("grp", "ep"), None),
            P(None, ("grp", "ep")),
            P(None, ("grp", "ep")),
            P("ep", None, "tp"),
            P("ep", None, "tp"),
            P("ep", "tp", None),
        ),
        out_specs=P(("grp", "ep"), "tp"),
        check_vma=False,
    )
```

```python
import functools

import jax
import jax.numpy as jnp
from jax import lax
from jax.experimental import pallas as pl
from jax.experimental.pallas import tpu as pltpu
from jax.sharding import PartitionSpec as P


VMEM = pl.BlockSpec(memory_space=pltpu.VMEM)
HBM = pl.BlockSpec(memory_space=pltpu.HBM)
F32 = jnp.float32
BF16 = jnp.bfloat16


def far_first(count):
    order, top = [], count // 2
    while top >= 1:
        order += range(top, 2 * top)
        top //= 2
    return order


def select_rows(ids, tokens):
    at = lax.broadcasted_iota(jnp.int32, (tokens.shape[0], ids.shape[1]), 0)
    onehot = (at == ids).astype(F32).astype(BF16)
    return lax.dot_general(
        onehot, tokens, (((0,), (0,)), ((), ())), preferred_element_type=F32
    ).astype(BF16)


def ids_of(picks_ref, expert, block):
    return lax.rem(picks_ref[pl.ds(expert, 1), :], block)


def first_gather_kernel(pair, picks_hbm, tokens_hbm, picks_ref, tokens_ref, out_ref, sems):
    copies = [
        pltpu.make_async_copy(picks_hbm, picks_ref, sems.at[0]),
        pltpu.make_async_copy(tokens_hbm, tokens_ref, sems.at[1]),
    ]
    for copy in copies:
        copy.start()
    for copy in copies:
        copy.wait()
    me, core = lax.axis_index("ep"), lax.axis_index("tp")
    ids = ids_of(picks_ref, me ^ (2 * pair + core), tokens_ref.shape[0])
    out_ref[...] = select_rows(ids, tokens_ref[...])


def gather_kernel(pairs, picks_ref, tokens_ref, *outs):
    block = tokens_ref.shape[0]
    me, core = lax.axis_index("ep"), lax.axis_index("tp")
    tokens = tokens_ref[...]
    half = picks_ref.shape[1] // 2
    for pair, out in zip(pairs, outs):
        out[...] = select_rows(ids_of(picks_ref, me ^ (2 * pair + core), block), tokens)
    near = select_rows(ids_of(picks_ref, me ^ 1, block), tokens)
    near_out, own_out = outs[-2:]
    near_out[...] = jnp.where(core == 0, near[:half], near[half:])
    own_out[...] = select_rows(ids_of(picks_ref, me, block), tokens)


def fetch_kernel(*refs):
    half = len(refs) // 2
    sems = refs[-1]
    pairs = list(zip(refs[:half], refs[half:-1]))
    for i, (src, dst) in enumerate(pairs):
        pltpu.make_async_copy(src, dst, sems.at[i]).start()
    for i, (src, dst) in enumerate(pairs):
        pltpu.make_async_copy(src, dst, sems.at[i]).wait()


def expert_kernel(count, *refs):
    gate_ref, up_ref, down_ref = refs[:3]
    own_ref, near_mine, near_other = refs[3:6]
    blocks = refs[6:6 + count - 2]
    keep_ref, send_ref, rows = refs[6 + count - 2:]
    core = lax.axis_index("tp")
    per = own_ref.shape[0]
    half = per // 2
    rows[:per, :] = own_ref[...]
    mine, other = near_mine[...], near_other[...]
    rows[per:per + half, :] = jnp.where(core == 0, mine, other)
    rows[per + half:2 * per, :] = jnp.where(core == 0, other, mine)
    pairs = count // 2 - 1
    for a in range(pairs):
        ours, theirs = blocks[a][...], blocks[pairs + a][...]
        rows[(2 + 2 * a) * per:(3 + 2 * a) * per, :] = jnp.where(core == 0, ours, theirs)
        rows[(3 + 2 * a) * per:(4 + 2 * a) * per, :] = jnp.where(core == 0, theirs, ours)
    x = rows[...]
    gate = jnp.dot(x, gate_ref[...], preferred_element_type=F32)
    up = jnp.dot(x, up_ref[...], preferred_element_type=F32)
    hidden = (gate / (1.0 + jnp.exp(-gate)) * up).astype(BF16)
    width = keep_ref.shape[1]
    for offset, out in ((1 - core, send_ref), (core, keep_ref)):
        columns = pl.ds(pl.multiple_of(offset * width, width), width)
        out[...] = jnp.dot(hidden, down_ref[:, columns], preferred_element_type=F32).astype(BF16)


def add_kernel(keep_ref, got_ref, *outs):
    per = outs[0].shape[0]
    for m, out in enumerate(outs):
        span = slice(m * per, (m + 1) * per)
        out[...] = (keep_ref[span, :].astype(F32) + got_ref[span, :].astype(F32)).astype(BF16)


def combine_kernel(picks_ref, weights_ref, *refs):
    blocks, out_ref, flat, mix = refs[:-3], refs[-3], refs[-2], refs[-1]
    me = lax.axis_index("ep")
    tokens, per = out_ref.shape[0], blocks[0].shape[0]
    for m, block in enumerate(blocks):
        expert = me ^ m
        flat[pl.ds(pl.multiple_of(expert * per, per), per), :] = block[...]
    at = lax.broadcasted_iota(jnp.int32, (tokens, picks_ref.shape[1]), 0)
    ids = lax.rem(picks_ref[...], tokens)
    mix[...] = jnp.where(at == ids, weights_ref[...].astype(F32), 0.0).astype(BF16)
    out_ref[...] = jnp.dot(mix[...], flat[...], preferred_element_type=F32).astype(BF16)


def call(kernel, outs, specs, scratch=(), flops=0, nbytes=0):
    return pl.pallas_call(
        kernel,
        out_shape=outs,
        in_specs=specs,
        out_specs=jax.tree.map(lambda _: VMEM, outs),
        scratch_shapes=list(scratch),
        cost_estimate=pl.CostEstimate(flops=flops, transcendentals=0, bytes_accessed=nbytes),
        compiler_params=pltpu.CompilerParams(vmem_limit_bytes=40 << 20),
    )


def shape(*dims, dtype=BF16):
    return jax.ShapeDtypeStruct(dims, dtype)


def per_device(tokens, picks, route_weights, gate_weight, up_weight, down_weight):
    count, cores = lax.axis_size("ep"), lax.axis_size("tp")
    experts, per = picks.shape
    block, width = tokens.shape
    if experts != count or cores != 2 or count & (count - 1) or count < 4:
        raise ValueError("unsupported mesh")
    wide = width // cores
    gate_weight, up_weight, down_weight = gate_weight[0], up_weight[0], down_weight[0]
    pairs = far_first(count // 2)

    def exchange(value, mask):
        return lax.ppermute(value, "ep", [(i, i ^ mask) for i in range(count)])

    def exchange_pair(value, pair):
        hops = [(i * 2 + t, (i ^ (2 * pair + t)) * 2 + t) for i in range(count) for t in range(2)]
        return lax.ppermute(value, ("ep", "tp"), hops)

    def swap(value):
        return lax.ppermute(value, "tp", [(0, 1), (1, 0)])

    n_far = len(pairs)
    in_hbm = lambda value: pltpu.with_memory_space_constraint(value, pltpu.HBM)
    local_picks, local_tokens, first = call(
        functools.partial(first_gather_kernel, pairs[0]),
        [pltpu.VMEM(picks.shape, picks.dtype), pltpu.VMEM(tokens.shape, BF16), shape(per, width)],
        [HBM, HBM],
        [pltpu.SemaphoreType.DMA((2,))],
    )(in_hbm(picks), in_hbm(tokens))
    sent = call(
        functools.partial(gather_kernel, pairs[1:]),
        [shape(per, width)] * (n_far - 1) + [shape(per // 2, width), shape(per, width)],
        [VMEM, VMEM],
    )(local_picks, local_tokens)
    got = {}
    for pair, value in zip(pairs, [first, *sent]):
        got[pair] = exchange_pair(value, pair)
    near, own = exchange(sent[-2], 1), sent[-1]
    other = {}
    for pair in pairs:
        other[pair] = swap(got[pair])
    near_other = swap(near)

    weights = call(
        fetch_kernel,
        [pltpu.VMEM(w.shape, w.dtype) for w in (gate_weight, up_weight, down_weight)],
        [HBM] * 3,
        [pltpu.SemaphoreType.DMA((3,))],
        nbytes=6 << 20,
    )(*map(in_hbm, (gate_weight, up_weight, down_weight)))

    order = sorted(pairs)
    keep, send = call(
        functools.partial(expert_kernel, count),
        [shape(count * per, wide)] * 2,
        [VMEM] * (6 + 2 * n_far),
        [pltpu.VMEM((count * per, width), BF16)],
        flops=2 * 3 * count * per * width * gate_weight.shape[1],
    )(*weights, own, near, near_other, *[got[a] for a in order], *[other[a] for a in order])
    received = swap(send)
    results = call(add_kernel, [shape(per, wide)] * count, [VMEM, VMEM])(keep, received)
    returned = [results[0]] + [None] * (count - 1)
    for mask in far_first(count):
        returned[mask] = exchange(results[mask], mask)
    return call(
        combine_kernel,
        shape(block, wide),
        [VMEM] * (2 + count),
        [pltpu.VMEM((count * per, wide), BF16), pltpu.VMEM((block, count * per), BF16)],
    )(picks.reshape(1, experts * per), route_weights.reshape(1, experts * per), *returned)


def solution(mesh):
    return jax.shard_map(
        per_device,
        mesh=mesh,
        in_specs=(
            P(("grp", "ep"), None),
            P(None, ("grp", "ep")),
            P(None, ("grp", "ep")),
            P("ep", None, "tp"),
            P("ep", None, "tp"),
            P("ep", "tp", None),
        ),
        out_specs=P(("grp", "ep"), "tp"),
        check_vma=False,
    )
```

```python
import functools

import jax
import jax.numpy as jnp
from jax import lax
from jax.experimental import pallas as pl
from jax.experimental.pallas import tpu as pltpu
from jax.sharding import PartitionSpec as P


VMEM = pl.BlockSpec(memory_space=pltpu.VMEM)
HBM = pl.BlockSpec(memory_space=pltpu.HBM)
F32 = jnp.float32
BF16 = jnp.bfloat16


def far_first(count):
    order, top = [], count // 2
    while top >= 1:
        order += range(top, 2 * top)
        top //= 2
    return order


def select_rows(ids, tokens):
    at = lax.broadcasted_iota(jnp.int32, (tokens.shape[0], ids.shape[1]), 0)
    onehot = (at == ids).astype(F32).astype(BF16)
    return lax.dot_general(
        onehot, tokens, (((0,), (0,)), ((), ())), preferred_element_type=F32
    ).astype(BF16)


def ids_of(picks_ref, expert, block):
    return lax.rem(picks_ref[pl.ds(expert, 1), :], block)


def first_gather_kernel(pair, picks_hbm, tokens_hbm, picks_ref, tokens_ref, out_ref, sems):
    copies = [
        pltpu.make_async_copy(picks_hbm, picks_ref, sems.at[0]),
        pltpu.make_async_copy(tokens_hbm, tokens_ref, sems.at[1]),
    ]
    for copy in copies:
        copy.start()
    for copy in copies:
        copy.wait()
    me, core = lax.axis_index("ep"), lax.axis_index("tp")
    ids = ids_of(picks_ref, me ^ (2 * pair + core), tokens_ref.shape[0])
    out_ref[...] = select_rows(ids, tokens_ref[...])


def gather_kernel(pairs, picks_ref, tokens_ref, *outs):
    block = tokens_ref.shape[0]
    me, core = lax.axis_index("ep"), lax.axis_index("tp")
    tokens = tokens_ref[...]
    masks = [2 * pair + core for pair in pairs] + [1, 0]
    for mask, out in zip(masks, outs):
        out[...] = select_rows(ids_of(picks_ref, me ^ mask, block), tokens)


def fetch_kernel(*refs):
    half = len(refs) // 2
    sems = refs[-1]
    pairs = list(zip(refs[:half], refs[half:-1]))
    for i, (src, dst) in enumerate(pairs):
        pltpu.make_async_copy(src, dst, sems.at[i]).start()
    for i, (src, dst) in enumerate(pairs):
        pltpu.make_async_copy(src, dst, sems.at[i]).wait()


def expert_kernel(n_local, n_pairs, *refs):
    gate_ref, up_ref, down_ref = refs[:3]
    local = refs[3:3 + n_local]
    blocks = refs[3 + n_local:3 + n_local + 2 * n_pairs]
    keep_ref, send_ref, rows = refs[-3:]
    core = lax.axis_index("tp")
    per = blocks[0].shape[0]
    for m, ref in enumerate(local):
        rows[m * per:(m + 1) * per, :] = ref[...]
    for i in range(n_pairs):
        base = (n_local + 2 * i) * per
        ours, theirs = blocks[i][...], blocks[n_pairs + i][...]
        rows[base:base + per, :] = jnp.where(core == 0, ours, theirs)
        rows[base + per:base + 2 * per, :] = jnp.where(core == 0, theirs, ours)
    x = rows[...]
    gate = jnp.dot(x, gate_ref[...], preferred_element_type=F32)
    up = jnp.dot(x, up_ref[...], preferred_element_type=F32)
    hidden = (gate / (1.0 + jnp.exp(-gate)) * up).astype(BF16)
    width = keep_ref.shape[1]
    for offset, out in ((1 - core, send_ref), (core, keep_ref)):
        columns = pl.ds(pl.multiple_of(offset * width, width), width)
        out[...] = jnp.dot(hidden, down_ref[:, columns], preferred_element_type=F32).astype(BF16)


def add_kernel(keep_ref, got_ref, *outs):
    per = outs[0].shape[0]
    for m, out in enumerate(outs):
        span = slice(m * per, (m + 1) * per)
        out[...] = (keep_ref[span, :].astype(F32) + got_ref[span, :].astype(F32)).astype(BF16)


def combine_kernel(picks_ref, weights_ref, *refs):
    blocks, out_ref, flat, mix = refs[:-3], refs[-3], refs[-2], refs[-1]
    me = lax.axis_index("ep")
    tokens, per = out_ref.shape[0], blocks[0].shape[0]
    for m, block in enumerate(blocks):
        expert = me ^ m
        flat[pl.ds(pl.multiple_of(expert * per, per), per), :] = block[...]
    at = lax.broadcasted_iota(jnp.int32, (tokens, picks_ref.shape[1]), 0)
    ids = lax.rem(picks_ref[...], tokens)
    mix[...] = jnp.where(at == ids, weights_ref[...].astype(F32), 0.0).astype(BF16)
    out_ref[...] = jnp.dot(mix[...], flat[...], preferred_element_type=F32).astype(BF16)


def call(kernel, outs, specs, scratch=(), flops=0, nbytes=0):
    return pl.pallas_call(
        kernel,
        out_shape=outs,
        in_specs=specs,
        out_specs=jax.tree.map(lambda _: VMEM, outs),
        scratch_shapes=list(scratch),
        cost_estimate=pl.CostEstimate(flops=flops, transcendentals=0, bytes_accessed=nbytes),
        compiler_params=pltpu.CompilerParams(vmem_limit_bytes=40 << 20),
    )


def shape(*dims, dtype=BF16):
    return jax.ShapeDtypeStruct(dims, dtype)


def chunks_of(count):
    pairs = far_first(count // 2)
    size = count // 8
    return pairs[:size], pairs[size:2 * size], pairs[2 * size:]


def per_device(tokens, picks, route_weights, gate_weight, up_weight, down_weight):
    count, cores = lax.axis_size("ep"), lax.axis_size("tp")
    experts, per = picks.shape
    block, width = tokens.shape
    if experts != count or cores != 2 or count & (count - 1) or count < 8:
        raise ValueError("unsupported mesh")
    wide = width // cores
    gate_weight, up_weight, down_weight = gate_weight[0], up_weight[0], down_weight[0]
    chunks = chunks_of(count)
    pairs = sum(chunks, [])
    in_hbm = lambda value: pltpu.with_memory_space_constraint(value, pltpu.HBM)

    def exchange(value, mask):
        return lax.ppermute(value, "ep", [(i, i ^ mask) for i in range(count)])

    def exchange_pair(value, pair):
        hops = [(i * 2 + t, (i ^ (2 * pair + t)) * 2 + t) for i in range(count) for t in range(2)]
        return lax.ppermute(value, ("ep", "tp"), hops)

    def swap(value):
        return lax.ppermute(value, "tp", [(0, 1), (1, 0)])

    local_picks, local_tokens, first = call(
        functools.partial(first_gather_kernel, pairs[0]),
        [pltpu.VMEM(picks.shape, picks.dtype), pltpu.VMEM(tokens.shape, BF16), shape(per, width)],
        [HBM, HBM],
        [pltpu.SemaphoreType.DMA((2,))],
    )(in_hbm(picks), in_hbm(tokens))
    *sent, near, own = call(
        functools.partial(gather_kernel, pairs[1:]),
        [shape(per, width)] * (len(pairs) + 1),
        [VMEM, VMEM],
    )(local_picks, local_tokens)
    got, other = {}, {}
    for pair, value in zip(pairs, [first, *sent]):
        got[pair] = exchange_pair(value, pair)
        other[pair] = swap(got[pair])
    near = exchange(near, 1)

    weights = call(
        fetch_kernel,
        [pltpu.VMEM(w.shape, w.dtype) for w in (gate_weight, up_weight, down_weight)],
        [HBM] * 3,
        [pltpu.SemaphoreType.DMA((3,))],
    )(*map(in_hbm, (gate_weight, up_weight, down_weight)))

    returned = [None] * count
    for name, chunk in zip("ABC", chunks):
        local = [own, near] if name == "C" else []
        masks = list(range(len(local))) + [2 * p + t for p in chunk for t in range(2)]
        rows = per * len(masks)
        keep, send = call(
            functools.partial(expert_kernel, len(local), len(chunk)),
            [shape(rows, wide)] * 2,
            [VMEM] * (3 + len(local) + 2 * len(chunk)),
            [pltpu.VMEM((rows, width), BF16)],
            flops=6 * rows * width * gate_weight.shape[1],
        )(*weights, *local, *[got[p] for p in chunk], *[other[p] for p in chunk])
        received = swap(send)
        results = call(add_kernel, [shape(per, wide)] * len(masks), [VMEM, VMEM])(keep, received)
        for mask, result in zip(masks, results):
            returned[mask] = exchange(result, mask) if mask else result
    return call(
        combine_kernel,
        shape(block, wide),
        [VMEM] * (2 + count),
        [pltpu.VMEM((count * per, wide), BF16), pltpu.VMEM((block, count * per), BF16)],
    )(local_picks.reshape(1, experts * per), route_weights.reshape(1, experts * per), *returned)


def solution(mesh):
    return jax.shard_map(
        per_device,
        mesh=mesh,
        in_specs=(
            P(("grp", "ep"), None),
            P(None, ("grp", "ep")),
            P(None, ("grp", "ep")),
            P("ep", None, "tp"),
            P("ep", None, "tp"),
            P("ep", "tp", None),
        ),
        out_specs=P(("grp", "ep"), "tp"),
        check_vma=False,
    )
```

```python
import functools

import jax
import jax.numpy as jnp
from jax import lax
from jax.experimental import pallas as pl
from jax.experimental.pallas import tpu as pltpu
from jax.sharding import PartitionSpec as P


VMEM = pl.BlockSpec(memory_space=pltpu.VMEM)
HBM = pl.BlockSpec(memory_space=pltpu.HBM)
F32 = jnp.float32
BF16 = jnp.bfloat16


def far_first(count):
    order, top = [], count // 2
    while top >= 1:
        order += range(top, 2 * top)
        top //= 2
    return order


def select_rows(ids, tokens):
    at = lax.broadcasted_iota(jnp.int32, (tokens.shape[0], ids.shape[1]), 0)
    onehot = (at == ids).astype(F32).astype(BF16)
    return lax.dot_general(
        onehot, tokens, (((0,), (0,)), ((), ())), preferred_element_type=F32
    ).astype(BF16)


def ids_of(picks_ref, expert, block):
    return lax.rem(picks_ref[pl.ds(expert, 1), :], block)


def first_gather_kernel(pair, picks_hbm, tokens_hbm, picks_ref, tokens_ref, out_ref, sems):
    copies = [
        pltpu.make_async_copy(picks_hbm, picks_ref, sems.at[0]),
        pltpu.make_async_copy(tokens_hbm, tokens_ref, sems.at[1]),
    ]
    for copy in copies:
        copy.start()
    for copy in copies:
        copy.wait()
    me, core = lax.axis_index("ep"), lax.axis_index("tp")
    ids = ids_of(picks_ref, me ^ (2 * pair + core), tokens_ref.shape[0])
    out_ref[...] = select_rows(ids, tokens_ref[...])


def gather_kernel(pairs, picks_ref, tokens_ref, *outs):
    block = tokens_ref.shape[0]
    me, core = lax.axis_index("ep"), lax.axis_index("tp")
    tokens = tokens_ref[...]
    masks = [2 * pair + core for pair in pairs] + [1, 0]
    for mask, out in zip(masks, outs):
        out[...] = select_rows(ids_of(picks_ref, me ^ mask, block), tokens)


def fetch_kernel(*refs):
    half = len(refs) // 2
    sems = refs[-1]
    pairs = list(zip(refs[:half], refs[half:-1]))
    for i, (src, dst) in enumerate(pairs):
        pltpu.make_async_copy(src, dst, sems.at[i]).start()
    for i, (src, dst) in enumerate(pairs):
        pltpu.make_async_copy(src, dst, sems.at[i]).wait()


def expert_kernel(n_local, n_pairs, by_rows, *refs):
    gate_ref, up_ref, down_ref = refs[:3]
    local = refs[3:3 + n_local]
    blocks = refs[3 + n_local:3 + n_local + 2 * n_pairs]
    keep_ref, send_ref, rows = refs[-3:]
    core = lax.axis_index("tp")
    per = blocks[0].shape[0]
    for m, ref in enumerate(local):
        rows[m * per:(m + 1) * per, :] = ref[...]
    for i in range(n_pairs):
        base = (n_local + 2 * i) * per
        ours, theirs = blocks[i][...], blocks[n_pairs + i][...]
        if not by_rows:
            ours, theirs = jnp.where(core == 0, ours, theirs), jnp.where(core == 0, theirs, ours)
        rows[base:base + per, :] = ours
        rows[base + per:base + 2 * per, :] = theirs
    x = rows[...]
    gate = jnp.dot(x, gate_ref[...], preferred_element_type=F32)
    up = jnp.dot(x, up_ref[...], preferred_element_type=F32)
    hidden = (gate / (1.0 + jnp.exp(-gate)) * up).astype(BF16)
    width = keep_ref.shape[1]
    split = per * (n_local if by_rows else n_local + 2 * n_pairs)
    for turn, offset in enumerate((1 - core, core)):
        columns = pl.ds(pl.multiple_of(offset * width, width), width)
        part = jnp.dot(hidden, down_ref[:, columns], preferred_element_type=F32).astype(BF16)
        if split:
            (send_ref, keep_ref)[turn][:split, :] = part[:split]
        for base in range(split, part.shape[0], 2 * per):
            mine, other = base + (1 - turn) * per, base + turn * per
            keep_ref[mine:mine + per, :] = part[base:base + per]
            send_ref[other:other + per, :] = part[base + per:base + 2 * per]


def add_kernel(keep_ref, got_ref, *outs):
    base = 0
    for out in outs:
        span = slice(base, base + out.shape[0])
        out[...] = (keep_ref[span, :].astype(F32) + got_ref[span, :].astype(F32)).astype(BF16)
        base += out.shape[0]


def combine_kernel(masks, pairs, picks_ref, weights_ref, *refs):
    blocks, out_ref, flat, mix = refs[:-3], refs[-3], refs[-2], refs[-1]
    me, core = lax.axis_index("ep"), lax.axis_index("tp")
    tokens, per = out_ref.shape[0], blocks[0].shape[0]

    def place(mask, value):
        flat[pl.ds(pl.multiple_of((me ^ mask) * per, per), per), :] = value

    for mask, block in zip(masks, blocks):
        place(mask, block[...])
    for i, pair in enumerate(pairs):
        direct, swapped = blocks[len(masks) + 2 * i:len(masks) + 2 * i + 2]
        place(2 * pair + core, direct[:per, :])
        place(2 * pair + 1 - core, swapped[per:, :])
    at = lax.broadcasted_iota(jnp.int32, (tokens, picks_ref.shape[1]), 0)
    ids = lax.rem(picks_ref[...], tokens)
    mix[...] = jnp.where(at == ids, weights_ref[...].astype(F32), 0.0).astype(BF16)
    out_ref[...] = jnp.dot(mix[...], flat[...], preferred_element_type=F32).astype(BF16)


def call(kernel, outs, specs, scratch=(), flops=0, nbytes=0):
    return pl.pallas_call(
        kernel,
        out_shape=outs,
        in_specs=specs,
        out_specs=jax.tree.map(lambda _: VMEM, outs),
        scratch_shapes=list(scratch),
        cost_estimate=pl.CostEstimate(flops=flops, transcendentals=0, bytes_accessed=nbytes),
        compiler_params=pltpu.CompilerParams(vmem_limit_bytes=40 << 20),
    )


def shape(*dims, dtype=BF16):
    return jax.ShapeDtypeStruct(dims, dtype)


def chunks_of(count):
    pairs = far_first(count // 2)
    size = count // 8
    return pairs[:size], pairs[size:2 * size], pairs[2 * size:]


def per_device(tokens, picks, route_weights, gate_weight, up_weight, down_weight):
    count, cores = lax.axis_size("ep"), lax.axis_size("tp")
    experts, per = picks.shape
    block, width = tokens.shape
    if experts != count or cores != 2 or count & (count - 1) or count < 8:
        raise ValueError("unsupported mesh")
    wide = width // cores
    gate_weight, up_weight, down_weight = gate_weight[0], up_weight[0], down_weight[0]
    chunks = chunks_of(count)
    pairs = chunks[0] + chunks[2] + chunks[1]
    in_hbm = lambda value: pltpu.with_memory_space_constraint(value, pltpu.HBM)

    def exchange(value, mask):
        return lax.ppermute(value, "ep", [(i, i ^ mask) for i in range(count)])

    def exchange_pair(value, pair):
        hops = [(i * 2 + t, (i ^ (2 * pair + t)) * 2 + t) for i in range(count) for t in range(2)]
        return lax.ppermute(value, ("ep", "tp"), hops)

    def swap(value):
        return lax.ppermute(value, "tp", [(0, 1), (1, 0)])

    local_picks, local_tokens, first = call(
        functools.partial(first_gather_kernel, pairs[0]),
        [pltpu.VMEM(picks.shape, picks.dtype), pltpu.VMEM(tokens.shape, BF16), shape(per, width)],
        [HBM, HBM],
        [pltpu.SemaphoreType.DMA((2,))],
    )(in_hbm(picks), in_hbm(tokens))
    *sent, near, own = call(
        functools.partial(gather_kernel, pairs[1:]),
        [shape(per, width)] * (len(pairs) + 1),
        [VMEM, VMEM],
    )(local_picks, local_tokens)
    got, other = {}, {}
    for pair, value in zip(pairs, [first, *sent]):
        got[pair] = exchange_pair(value, pair)
        other[pair] = swap(got[pair])
    near = exchange(near, 1)

    weights = call(
        fetch_kernel,
        [pltpu.VMEM(w.shape, w.dtype) for w in (gate_weight, up_weight, down_weight)],
        [HBM] * 3,
        [pltpu.SemaphoreType.DMA((3,))],
    )(*map(in_hbm, (gate_weight, up_weight, down_weight)))

    masks, direct, by_pair = [], [], []
    for name, chunk in zip("ABC", chunks):
        local = [own, near] if name == "C" else []
        by_rows = name != "B"
        rows = per * (len(local) + 2 * len(chunk))
        keep, send = call(
            functools.partial(expert_kernel, len(local), len(chunk), by_rows),
            [shape(rows, wide)] * 2,
            [VMEM] * (3 + len(local) + 2 * len(chunk)),
            [pltpu.VMEM((rows, width), BF16)],
            flops=6 * rows * width * gate_weight.shape[1],
        )(*weights, *local, *[got[p] for p in chunk], *[other[p] for p in chunk])
        received = swap(send)
        singles = [0, 1] if name == "C" else []
        singles += [] if by_rows else [2 * p + t for p in chunk for t in range(2)]
        outs = [shape(per, wide)] * len(singles)
        outs += [shape(2 * per, wide)] * len(chunk) if by_rows else []
        results = call(add_kernel, outs, [VMEM, VMEM])(keep, received)
        for mask, result in zip(singles, results):
            direct.append(exchange(result, mask) if mask else result)
            masks.append(mask)
        for pair, result in zip(chunk, results[len(singles):]):
            came = exchange_pair(result, pair)
            by_pair += [came, swap(came)]
    return call(
        functools.partial(combine_kernel, masks, chunks[0] + chunks[2]),
        shape(block, wide),
        [VMEM] * (2 + len(direct) + len(by_pair)),
        [pltpu.VMEM((count * per, wide), BF16), pltpu.VMEM((block, count * per), BF16)],
    )(
        local_picks.reshape(1, experts * per),
        route_weights.reshape(1, experts * per),
        *direct,
        *by_pair,
    )


def solution(mesh):
    return jax.shard_map(
        per_device,
        mesh=mesh,
        in_specs=(
            P(("grp", "ep"), None),
            P(None, ("grp", "ep")),
            P(None, ("grp", "ep")),
            P("ep", None, "tp"),
            P("ep", None, "tp"),
            P("ep", "tp", None),
        ),
        out_specs=P(("grp", "ep"), "tp"),
        check_vma=False,
    )
```

```python
import functools

import jax
import jax.numpy as jnp
from jax import lax
from jax.experimental import pallas as pl
from jax.experimental.pallas import tpu as pltpu
from jax.sharding import PartitionSpec as P


VMEM = pl.BlockSpec(memory_space=pltpu.VMEM)
HBM = pl.BlockSpec(memory_space=pltpu.HBM)
F32 = jnp.float32
BF16 = jnp.bfloat16


def one_hot(ids, block):
    at = lax.broadcasted_iota(jnp.int32, (block, ids.shape[1]), 0)
    return (at == ids).astype(F32).astype(BF16)


def select_rows(onehot, tokens):
    return lax.dot_general(
        onehot, tokens, (((0,), (0,)), ((), ())), preferred_element_type=F32
    ).astype(BF16)


def ids_of(picks_ref, expert, block):
    return lax.rem(picks_ref[pl.ds(expert, 1), :], block)


def mask_of(pair):
    return jnp.where(lax.axis_index("tp") == 0, *pair)


def first_gather_kernel(pair, parts, picks_hbm, tokens_hbm, picks_ref, tokens_ref, out_ref, sems):
    block, width = tokens_ref.shape
    step = width // parts
    copies = [pltpu.make_async_copy(picks_hbm, picks_ref, sems.at[parts])]
    for i in range(parts):
        span = slice(i * step, (i + 1) * step)
        copies.append(
            pltpu.make_async_copy(tokens_hbm.at[:, span], tokens_ref.at[:, span], sems.at[i])
        )
    for copy in copies:
        copy.start()
    copies[0].wait()
    ids = ids_of(picks_ref, lax.axis_index("ep") ^ mask_of(pair), block)
    onehot = one_hot(ids, block)
    for i in range(parts):
        copies[i + 1].wait()
        span = slice(i * step, (i + 1) * step)
        out_ref[:, span] = select_rows(onehot, tokens_ref[:, span])


def gather_kernel(pairs, picks_ref, tokens_ref, *refs):
    outs, onehot = refs[:-1], refs[-1]
    block, per = tokens_ref.shape[0], picks_ref.shape[1]
    me = lax.axis_index("ep")
    masks = [mask_of(pair) for pair in pairs] + [1, 0]
    for i, mask in enumerate(masks):
        onehot[:, i * per:(i + 1) * per] = one_hot(ids_of(picks_ref, me ^ mask, block), block)
    rows = select_rows(onehot[...], tokens_ref[...])
    for i, out in enumerate(outs):
        out[...] = rows[i * per:(i + 1) * per]


def fetch_kernel(*refs):
    half = len(refs) // 2
    sems = refs[-1]
    pairs = list(zip(refs[:half], refs[half:-1]))
    for i, (src, dst) in enumerate(pairs):
        pltpu.make_async_copy(src, dst, sems.at[i]).start()
    for i, (src, dst) in enumerate(pairs):
        pltpu.make_async_copy(src, dst, sems.at[i]).wait()


def expert_kernel(n_local, apart, *refs):
    weights, rows = refs[:6], refs[-1]
    n_blocks = next(i for i, ref in enumerate(refs[6:]) if ref.shape[1] != refs[6].shape[1])
    blocks, outs = refs[6:6 + n_blocks], refs[6 + n_blocks:-1]
    core = lax.axis_index("tp")
    per = blocks[0].shape[0]
    for i, block in enumerate(blocks):
        rows[i * per:(i + 1) * per, :] = block[...]
    used = n_blocks * per
    if rows.shape[0] > used:
        rows[used:, :] = jnp.zeros((rows.shape[0] - used, rows.shape[1]), BF16)
    x, hidden = rows[...], []
    for gate_ref, up_ref in (weights[0:2], weights[3:5]):
        gate = jnp.dot(x, gate_ref[...], preferred_element_type=F32)
        up = jnp.dot(x, up_ref[...], preferred_element_type=F32)
        hidden.append((gate / (1.0 + jnp.exp(-gate)) * up).astype(BF16))
    width = outs[0].shape[1]
    for turn, offset in enumerate((core, 1 - core)):
        columns = pl.ds(pl.multiple_of(offset * width, width), width)
        part = sum(
            jnp.dot(half, down_ref[:, columns], preferred_element_type=F32)
            for half, down_ref in zip(hidden, (weights[2], weights[5]))
        ).astype(BF16)
        for i in range(n_blocks):
            value = part[i * per:(i + 1) * per]
            if i < n_local:
                if turn == 0:
                    outs[i][...] = value
            elif apart:
                outs[n_local + 2 * (i - n_local) + turn][...] = value
            else:
                outs[i][turn * per:(turn + 1) * per, :] = value


def mix_kernel(groups, picks_ref, weights_ref, *refs):
    outs, scale = refs[:-1], refs[-1]
    me = lax.axis_index("ep")
    per = picks_ref.shape[1]
    scale[...] = weights_ref[...].astype(F32)
    for masks, out in zip(groups, outs):
        at = lax.broadcasted_iota(jnp.int32, (out.shape[0], per), 0)
        for i, mask in enumerate(masks):
            ids = ids_of(picks_ref, me ^ mask, out.shape[0])
            row = scale[pl.ds(me ^ mask, 1), :]
            out[:, i * per:(i + 1) * per] = jnp.where(at == ids, row, 0.0).astype(BF16)


def lay(flat, singles, pairs):
    core = lax.axis_index("tp")
    per = flat.shape[0] // (len(singles) + len(pairs))
    for i, block in enumerate(singles):
        flat[i * per:(i + 1) * per, :] = block[...]
    for i in range(0, len(pairs), 2):
        base = (len(singles) + i) * per
        other = pairs[i + 1]
        ours, theirs = pairs[i][:per, :], other[other.shape[0] - per:, :]
        flat[base:base + per, :] = jnp.where(core == 0, ours, theirs)
        flat[base + per:base + 2 * per, :] = jnp.where(core == 0, theirs, ours)


def combine_kernel(n_singles, mix_ref, *refs):
    blocks, acc_ref, flat = refs[:-2], refs[-2], refs[-1]
    lay(flat, blocks[:n_singles], blocks[n_singles:])
    acc_ref[...] = jnp.dot(mix_ref[...], flat[...], preferred_element_type=F32)


def finish_kernel(n_singles, steps, mix_ref, acc_ref, *refs):
    blocks, (out_hbm, flat, out, sems) = refs[:-4], refs[-4:]
    lay(flat, blocks[:n_singles], blocks[n_singles:])
    rows = out.shape[0] // steps
    copies = []
    for i in range(steps):
        span = slice(i * rows, (i + 1) * rows)
        last = jnp.dot(mix_ref[span, :], flat[...], preferred_element_type=F32)
        out[span, :] = (acc_ref[span, :] + last).astype(BF16)
        copies.append(pltpu.make_async_copy(out.at[span, :], out_hbm.at[span, :], sems.at[i]))
        copies[-1].start()
    for copy in copies:
        copy.wait()


def call(kernel, outs, specs, scratch=(), flops=0, out_specs=None):
    return pl.pallas_call(
        kernel,
        out_shape=outs,
        in_specs=specs,
        out_specs=out_specs or jax.tree.map(lambda _: VMEM, outs),
        scratch_shapes=list(scratch),
        cost_estimate=pl.CostEstimate(flops=flops, transcendentals=0, bytes_accessed=0),
        compiler_params=pltpu.CompilerParams(vmem_limit_bytes=40 << 20),
    )


def shape(*dims, dtype=BF16):
    return jax.ShapeDtypeStruct(dims, dtype)


def chunks_of(count):
    top, far, rest = count // 2, [], []
    while top > 1:
        pairs = [(m, m + 1) for m in range(top, 2 * top, 2)]
        (rest.extend if far else far.extend)(pairs)
        top //= 2
    return {"A": far[:len(far) // 2], "B": far[len(far) // 2:], "C": rest}


def per_device(tokens, picks, route_weights, gate_weight, up_weight, down_weight):
    count, cores = lax.axis_size("ep"), lax.axis_size("tp")
    experts, per = picks.shape
    block, width = tokens.shape
    if experts != count or cores != 2 or count & (count - 1) or count < 8:
        raise ValueError("unsupported mesh")
    wide = width // cores
    gate_weight, up_weight, down_weight = gate_weight[0], up_weight[0], down_weight[0]
    chunks = chunks_of(count)
    pairs = chunks["A"] + chunks["C"] + chunks["B"]
    in_hbm = lambda value: pltpu.with_memory_space_constraint(value, pltpu.HBM)

    def exchange(value, mask):
        return lax.ppermute(value, "ep", [(i, i ^ mask) for i in range(count)])

    def exchange_pair(value, pair, cross=False):
        hops = [
            (i * 2 + t, (i ^ pair[t]) * 2 + (t ^ cross)) for i in range(count) for t in range(2)
        ]
        return lax.ppermute(value, ("ep", "tp"), hops)

    def swap(value):
        return lax.ppermute(value, "tp", [(0, 1), (1, 0)])

    local_picks, local_tokens, first = call(
        functools.partial(first_gather_kernel, pairs[0], 1),
        [pltpu.VMEM(picks.shape, picks.dtype), pltpu.VMEM(tokens.shape, BF16), shape(per, width)],
        [HBM, HBM],
        [pltpu.SemaphoreType.DMA((2,))],
    )(in_hbm(picks), in_hbm(tokens))
    *sent, near, own = call(
        functools.partial(gather_kernel, pairs[1:]),
        [shape(per, width)] * (len(pairs) + 1),
        [VMEM, VMEM],
        [pltpu.VMEM((block, per * (len(pairs) + 1)), BF16)],
    )(local_picks, local_tokens)
    got = {}
    for pair, value in zip(pairs, [first, *sent]):
        got[pair] = exchange_pair(value, pair)
    near = exchange(near, 1)

    weights = call(
        fetch_kernel,
        [pltpu.VMEM(w.shape, w.dtype) for w in (up_weight, down_weight)],
        [HBM] * 2,
        [pltpu.SemaphoreType.DMA((2,))],
    )(*map(in_hbm, (up_weight, down_weight)))
    weights = [gate_weight, *weights]
    for weight in (gate_weight, up_weight, down_weight):
        weights.append(swap(weight))

    returned, by_pair = {}, []
    for locals_at, names, apart in CALLS:
        local = [(own, near)[m] for m in locals_at]
        chunk = [pair for name in names for pair in chunks[name]]
        outs = [shape(per, wide)] * len(local)
        outs += [shape(per, wide)] * (2 * len(chunk)) if apart else [shape(2 * per, wide)] * len(chunk)
        rows = per * (len(local) + len(chunk))
        results = call(
            functools.partial(expert_kernel, len(local), apart),
            outs,
            [VMEM] * (6 + len(local) + len(chunk)),
            [pltpu.VMEM((max(rows, 128), width), BF16)],
            flops=12 * rows * width * gate_weight.shape[1],
        )(*weights, *local, *[got[pair] for pair in chunk])
        for mask, result in zip(locals_at, results):
            returned[mask] = exchange(result, mask) if mask else result
        results = results[len(local):]
        for i, pair in enumerate(chunk):
            if apart:
                ours = exchange_pair(results[2 * i], pair)
                theirs = exchange_pair(results[2 * i + 1], pair, True)
            else:
                ours = exchange_pair(results[i], pair)
                theirs = swap(ours)
            by_pair.append((pair, ours, theirs))
    is_late = lambda masks: masks[0] == 1 or masks in chunks["B"]
    groups = []
    for late in (False, True):
        singles = [m for m in returned if is_late((m,)) == late]
        pairs = [entry for entry in by_pair if is_late(entry[0]) == late]
        masks = singles + [m for pair, _, _ in pairs for m in pair]
        blocks = [returned[m] for m in singles]
        blocks += [value for _, *values in pairs for value in values]
        groups.append((masks, len(singles), blocks))
    (early, n_early, early_blocks), (late, n_late, late_blocks) = groups
    mix_early, mix_late = call(
        functools.partial(mix_kernel, (early, late)),
        [shape(block, len(early) * per), shape(block, len(late) * per)],
        [VMEM, VMEM],
        [pltpu.VMEM(route_weights.shape, F32)],
    )(local_picks, route_weights)
    acc = call(
        functools.partial(combine_kernel, n_early),
        shape(block, wide, dtype=F32),
        [VMEM] * (1 + len(early_blocks)),
        [pltpu.VMEM((len(early) * per, wide), BF16)],
    )(mix_early, *early_blocks)
    return call(
        functools.partial(finish_kernel, n_late, STEPS),
        shape(block, wide),
        [VMEM] * (2 + len(late_blocks)),
        [
            pltpu.VMEM((len(late) * per, wide), BF16),
            pltpu.VMEM((block, wide), BF16),
            pltpu.SemaphoreType.DMA((STEPS,)),
        ],
        out_specs=HBM,
    )(mix_late, acc, *late_blocks)


CALLS = (((), "AC", False), ((0, 1), "B", True))
STEPS = 4


def solution(mesh):
    return jax.shard_map(
        per_device,
        mesh=mesh,
        in_specs=(
            P(("grp", "ep"), None),
            P(None, ("grp", "ep")),
            P(None, ("grp", "ep")),
            P("ep", None, "tp"),
            P("ep", None, "tp"),
            P("ep", "tp", None),
        ),
        out_specs=P(("grp", "ep"), "tp"),
        check_vma=False,
    )
```

```python
import functools

import jax
import jax.numpy as jnp
from jax import lax
from jax.experimental import pallas as pl
from jax.experimental.pallas import tpu as pltpu
from jax.sharding import PartitionSpec as P


VMEM = pl.BlockSpec(memory_space=pltpu.VMEM)
HBM = pl.BlockSpec(memory_space=pltpu.HBM)
F32 = jnp.float32
BF16 = jnp.bfloat16


def one_hot(ids, block):
    at = lax.broadcasted_iota(jnp.int32, (block, ids.shape[1]), 0)
    return (at == ids).astype(F32).astype(BF16)


def select_rows(onehot, tokens):
    return lax.dot_general(
        onehot, tokens, (((0,), (0,)), ((), ())), preferred_element_type=F32
    ).astype(BF16)


def ids_of(picks_ref, expert, block):
    return lax.rem(picks_ref[pl.ds(expert, 1), :], block)


def mask_of(pair):
    return jnp.where(lax.axis_index("tp") == 0, *pair)


def first_gather_kernel(pair, parts, picks_hbm, tokens_hbm, picks_ref, tokens_ref, out_ref, sems):
    block, width = tokens_ref.shape
    step = width // parts
    copies = [pltpu.make_async_copy(picks_hbm, picks_ref, sems.at[parts])]
    for i in range(parts):
        span = slice(i * step, (i + 1) * step)
        copies.append(
            pltpu.make_async_copy(tokens_hbm.at[:, span], tokens_ref.at[:, span], sems.at[i])
        )
    for copy in copies:
        copy.start()
    copies[0].wait()
    ids = ids_of(picks_ref, lax.axis_index("ep") ^ mask_of(pair), block)
    onehot = one_hot(ids, block)
    for i in range(parts):
        copies[i + 1].wait()
        span = slice(i * step, (i + 1) * step)
        out_ref[:, span] = select_rows(onehot, tokens_ref[:, span])


def gather_kernel(pairs, picks_ref, tokens_ref, *refs):
    outs, onehot = refs[:-1], refs[-1]
    block, per = tokens_ref.shape[0], picks_ref.shape[1]
    me = lax.axis_index("ep")
    masks = [mask_of(pair) for pair in pairs] + [1, 0]
    for i, mask in enumerate(masks):
        onehot[:, i * per:(i + 1) * per] = one_hot(ids_of(picks_ref, me ^ mask, block), block)
    rows = select_rows(onehot[...], tokens_ref[...])
    for i, out in enumerate(outs):
        out[...] = rows[i * per:(i + 1) * per]


def fetch_kernel(*refs):
    half = len(refs) // 2
    sems = refs[-1]
    pairs = list(zip(refs[:half], refs[half:-1]))
    for i, (src, dst) in enumerate(pairs):
        pltpu.make_async_copy(src, dst, sems.at[i]).start()
    for i, (src, dst) in enumerate(pairs):
        pltpu.make_async_copy(src, dst, sems.at[i]).wait()


def expert_kernel(n_local, apart, *refs):
    weights, rows = refs[:6], refs[-1]
    n_blocks = next(i for i, ref in enumerate(refs[6:]) if ref.shape[1] != refs[6].shape[1])
    blocks, outs = refs[6:6 + n_blocks], refs[6 + n_blocks:-1]
    core = lax.axis_index("tp")
    per = blocks[0].shape[0]
    for i, block in enumerate(blocks):
        rows[i * per:(i + 1) * per, :] = block[...]
    used = n_blocks * per
    if rows.shape[0] > used:
        rows[used:, :] = jnp.zeros((rows.shape[0] - used, rows.shape[1]), BF16)
    x, hidden = rows[...], []
    for gate_ref, up_ref in (weights[0:2], weights[3:5]):
        gate = jnp.dot(x, gate_ref[...], preferred_element_type=F32)
        up = jnp.dot(x, up_ref[...], preferred_element_type=F32)
        hidden.append((gate / (1.0 + jnp.exp(-gate)) * up).astype(BF16))
    width = outs[0].shape[1]
    for turn, offset in enumerate((core, 1 - core)):
        columns = pl.ds(pl.multiple_of(offset * width, width), width)
        part = sum(
            jnp.dot(half, down_ref[:, columns], preferred_element_type=F32)
            for half, down_ref in zip(hidden, (weights[2], weights[5]))
        ).astype(BF16)
        for i in range(n_blocks):
            value = part[i * per:(i + 1) * per]
            if i < n_local:
                if turn == 0:
                    outs[i][...] = value
            elif apart:
                outs[n_local + 2 * (i - n_local) + turn][...] = value
            else:
                outs[i][turn * per:(turn + 1) * per, :] = value


def mix_kernel(groups, picks_ref, weights_ref, *refs):
    outs, scale = refs[:-1], refs[-1]
    me = lax.axis_index("ep")
    per = picks_ref.shape[1]
    scale[...] = weights_ref[...].astype(F32)
    for masks, out in zip(groups, outs):
        at = lax.broadcasted_iota(jnp.int32, (out.shape[0], per), 0)
        for i, mask in enumerate(masks):
            ids = ids_of(picks_ref, me ^ mask, out.shape[0])
            row = scale[pl.ds(me ^ mask, 1), :]
            out[:, i * per:(i + 1) * per] = jnp.where(at == ids, row, 0.0).astype(BF16)


def lay(flat, singles, pairs):
    core = lax.axis_index("tp")
    per = flat.shape[0] // (len(singles) + len(pairs))
    for i, block in enumerate(singles):
        flat[i * per:(i + 1) * per, :] = block[...]
    for i in range(0, len(pairs), 2):
        base = (len(singles) + i) * per
        other = pairs[i + 1]
        ours, theirs = pairs[i][:per, :], other[other.shape[0] - per:, :]
        flat[base:base + per, :] = jnp.where(core == 0, ours, theirs)
        flat[base + per:base + 2 * per, :] = jnp.where(core == 0, theirs, ours)


def combine_kernel(n_singles, mix_ref, *refs):
    blocks, acc_ref, flat = refs[:-2], refs[-2], refs[-1]
    lay(flat, blocks[:n_singles], blocks[n_singles:])
    acc_ref[...] = jnp.dot(mix_ref[...], flat[...], preferred_element_type=F32)


def finish_kernel(n_singles, steps, mix_ref, acc_ref, *refs):
    blocks, (out_hbm, flat, out, sems) = refs[:-4], refs[-4:]
    lay(flat, blocks[:n_singles], blocks[n_singles:])
    width = out.shape[1] // steps
    copies = []
    for i in range(steps):
        span = slice(i * width, (i + 1) * width)
        last = jnp.dot(mix_ref[...], flat[:, span], preferred_element_type=F32)
        out[:, span] = (acc_ref[:, span] + last).astype(BF16)
        copies.append(pltpu.make_async_copy(out.at[:, span], out_hbm.at[:, span], sems.at[i]))
        copies[-1].start()
    for copy in copies:
        copy.wait()


def call(kernel, outs, specs, scratch=(), flops=0, out_specs=None):
    return pl.pallas_call(
        kernel,
        out_shape=outs,
        in_specs=specs,
        out_specs=out_specs or jax.tree.map(lambda _: VMEM, outs),
        scratch_shapes=list(scratch),
        cost_estimate=pl.CostEstimate(flops=flops, transcendentals=0, bytes_accessed=0),
        compiler_params=pltpu.CompilerParams(vmem_limit_bytes=40 << 20),
    )


def shape(*dims, dtype=BF16):
    return jax.ShapeDtypeStruct(dims, dtype)


def chunks_of(count):
    top, far, rest = count // 2, [], []
    while top > 1:
        pairs = [(m, m + 1) for m in range(top, 2 * top, 2)]
        (rest.extend if far else far.extend)(pairs)
        top //= 2
    rest = [pair[::-1] for pair in rest]
    return {"A": far[:len(far) // 2], "B": far[len(far) // 2:], "C": rest}


def per_device(tokens, picks, route_weights, gate_weight, up_weight, down_weight):
    count, cores = lax.axis_size("ep"), lax.axis_size("tp")
    experts, per = picks.shape
    block, width = tokens.shape
    if experts != count or cores != 2 or count & (count - 1) or count < 8:
        raise ValueError("unsupported mesh")
    wide = width // cores
    gate_weight, up_weight, down_weight = gate_weight[0], up_weight[0], down_weight[0]
    chunks = chunks_of(count)
    pairs = chunks["A"] + chunks["C"] + chunks["B"]
    in_hbm = lambda value: pltpu.with_memory_space_constraint(value, pltpu.HBM)

    def exchange(value, mask):
        return lax.ppermute(value, "ep", [(i, i ^ mask) for i in range(count)])

    def exchange_pair(value, pair, cross=False):
        hops = [
            (i * 2 + t, (i ^ pair[t]) * 2 + (t ^ cross)) for i in range(count) for t in range(2)
        ]
        return lax.ppermute(value, ("ep", "tp"), hops)

    def swap(value):
        return lax.ppermute(value, "tp", [(0, 1), (1, 0)])

    local_picks, local_tokens, first = call(
        functools.partial(first_gather_kernel, pairs[0], 1),
        [pltpu.VMEM(picks.shape, picks.dtype), pltpu.VMEM(tokens.shape, BF16), shape(per, width)],
        [HBM, HBM],
        [pltpu.SemaphoreType.DMA((2,))],
    )(in_hbm(picks), in_hbm(tokens))
    *sent, near, own = call(
        functools.partial(gather_kernel, pairs[1:]),
        [shape(per, width)] * (len(pairs) + 1),
        [VMEM, VMEM],
        [pltpu.VMEM((block, per * (len(pairs) + 1)), BF16)],
    )(local_picks, local_tokens)
    got = {}
    for pair, value in zip(pairs, [first, *sent]):
        got[pair] = exchange_pair(value, pair)
    near = exchange(near, 1)

    weights = call(
        fetch_kernel,
        [pltpu.VMEM(w.shape, w.dtype) for w in (up_weight, down_weight)],
        [HBM] * 2,
        [pltpu.SemaphoreType.DMA((2,))],
    )(*map(in_hbm, (up_weight, down_weight)))
    weights = [gate_weight, *weights]
    for weight in (gate_weight, up_weight, down_weight):
        weights.append(swap(weight))

    returned, by_pair = {}, []
    for locals_at, names, apart in CALLS:
        local = [(own, near)[m] for m in locals_at]
        chunk = [pair for name in names for pair in chunks[name]]
        outs = [shape(per, wide)] * len(local)
        outs += [shape(per, wide)] * (2 * len(chunk)) if apart else [shape(2 * per, wide)] * len(chunk)
        rows = per * (len(local) + len(chunk))
        results = call(
            functools.partial(expert_kernel, len(local), apart),
            outs,
            [VMEM] * (6 + len(local) + len(chunk)),
            [pltpu.VMEM((max(rows, 128), width), BF16)],
            flops=12 * rows * width * gate_weight.shape[1],
        )(*weights, *local, *[got[pair] for pair in chunk])
        for mask, result in zip(locals_at, results):
            returned[mask] = exchange(result, mask) if mask else result
        results = results[len(local):]
        for i, pair in enumerate(chunk):
            if apart:
                ours = exchange_pair(results[2 * i], pair)
                theirs = exchange_pair(results[2 * i + 1], pair, True)
            else:
                ours = exchange_pair(results[i], pair)
                theirs = swap(ours)
            by_pair.append((pair, ours, theirs))
    is_late = lambda masks: masks[0] == 1 or masks in chunks["B"]
    groups = []
    for late in (False, True):
        singles = [m for m in returned if is_late((m,)) == late]
        pairs = [entry for entry in by_pair if is_late(entry[0]) == late]
        masks = singles + [m for pair, _, _ in pairs for m in pair]
        blocks = [returned[m] for m in singles]
        blocks += [value for _, *values in pairs for value in values]
        groups.append((masks, len(singles), blocks))
    (early, n_early, early_blocks), (late, n_late, late_blocks) = groups
    mix_early, mix_late = call(
        functools.partial(mix_kernel, (early, late)),
        [shape(block, len(early) * per), shape(block, len(late) * per)],
        [VMEM, VMEM],
        [pltpu.VMEM(route_weights.shape, F32)],
    )(local_picks, route_weights)
    acc = call(
        functools.partial(combine_kernel, n_early),
        shape(block, wide, dtype=F32),
        [VMEM] * (1 + len(early_blocks)),
        [pltpu.VMEM((len(early) * per, wide), BF16)],
    )(mix_early, *early_blocks)
    return call(
        functools.partial(finish_kernel, n_late, STEPS),
        shape(block, wide),
        [VMEM] * (2 + len(late_blocks)),
        [
            pltpu.VMEM((len(late) * per, wide), BF16),
            pltpu.VMEM((block, wide), BF16),
            pltpu.SemaphoreType.DMA((STEPS,)),
        ],
        out_specs=HBM,
    )(mix_late, acc, *late_blocks)


CALLS = (((), "AC", False), ((0, 1), "B", True))
STEPS = 2


def solution(mesh):
    return jax.shard_map(
        per_device,
        mesh=mesh,
        in_specs=(
            P(("grp", "ep"), None),
            P(None, ("grp", "ep")),
            P(None, ("grp", "ep")),
            P("ep", None, "tp"),
            P("ep", None, "tp"),
            P("ep", "tp", None),
        ),
        out_specs=P(("grp", "ep"), "tp"),
        check_vma=False,
    )
```
